32 devices in a mesh: sp: 4 (over y, x), tp: 8 (over z, core).
Axes of the slice: x: 2, y: 2, z: 4, core: 2. Of those that a mesh axis runs over, the one named last changes fastest.
Arguments:
- query_vectors: bfloat16 [4096, 16, 128], P('sp', 'tp'), may hold values from -6 to 6
- key_vectors: bfloat16 [4096, 16, 128], P('sp', 'tp'), may hold values from -6 to 6
- value_vectors: bfloat16 [4096, 16, 128], P('sp', 'tp'), may hold values from -6 to 6
- out_gate: bfloat16 [4096, 16, 128], P('sp', 'tp'), may hold values from -6 to 6
- decay_rate: float32 [2, 16], P(None, 'tp'), may hold values from 0 to 1
- decay_pre: float32 [2, 16, 4096], P(None, 'tp', 'sp'), may hold values from -6 to 6
- decay_shock: float32 [2, 16, 4096], P(None, 'tp', 'sp'), may hold values from -2 to 0
- beta_pre: float32 [2, 16, 4096], P(None, 'tp', 'sp'), may hold values from -12 to 0
- head_gain: float32 [128], replicated, may hold values from 0.1 to 1.9
- w_out: bfloat16 [2048, 2048], P('tp'), may hold values from -0.125 to 0.125
- tokens: bfloat16 [4096, 2048], P(('sp', 'tp')), may hold values from -6 to 6
- norm_gain: float32 [2048], replicated, may hold values from 0.1 to 1.9
- experts_pick: int32 [4096, 2], P(('sp', 'tp')), may hold values from 0 to 3, as said below
- pair_logits: float32 [4096, 2], P(('sp', 'tp')), may hold values from -6 to 6
- group_logits: float32 [4096, 2], P(('sp', 'tp')), may hold values from -6 to 6
- expert_gate: bfloat16 [4, 2048, 2048], P('sp', None, 'tp'), may hold values from -0.125 to 0.125
- expert_up: bfloat16 [4, 2048, 2048], P('sp', None, 'tp'), may hold values from -0.125 to 0.125
- expert_down: bfloat16 [4, 2048, 2048], P('sp', None, 'tp'), may hold values from -0.5 to 0.5
Outputs:
- layer_out: bfloat16 [4096, 2048], P(('sp', 'tp'))
The draws below stay inside these ranges and needn't reach their ends.
Inputs may be any that keep to these rules, and one draw needn't show every extreme that they name: `experts_pick`: each token names two different experts of one group of 2 consecutive experts. The 128 tokens of one device fall 64 into each group. At most 64 tokens of one device name any one expert, and in every draw every expert is named by 64 tokens of every device.
All inputs are finite; a program needn't handle non-finite values.
Results may differ from the reference program's by a relative error of at most 0.02.
Values may be sent and summed in bfloat16 or wider, within the bound.
A program may use at most 128 MiB of HBM per device.

```python
import jax
import jax.numpy as jnp
from jax import lax

D = 2048
HEADS = 16
HEAD_DIM = 128
BLOCK = 64
EXP_FF = 2048
GROUP_SIZE = 2
TOK_SP = 1024
SEQ = 4096
TOK_DEV = 128
EXPERTS = 4
EXPERT_GROUPS = 2
CAP = 64
N_TP = 8


def draw_decay_rate(key, part):
    pick_key, slow_key, fast_key = jax.random.split(key, 3)
    chance = jax.random.uniform(pick_key, (2, HEADS), jnp.float32)
    slow_mask = chance < 0.5
    slow_rate = jnp.exp(jax.random.uniform(slow_key, (2, HEADS), jnp.float32, jnp.log(0.15), jnp.log(0.6))) / SEQ
    fast_rate = jnp.exp(jax.random.uniform(fast_key, (2, HEADS), jnp.float32, jnp.log(0.03), jnp.log(0.08)))
    return jnp.where(slow_mask, slow_rate, fast_rate).astype(jnp.float32)


def draw_decay_pre(key, part):
    noise_key, level_key = jax.random.split(key)
    block_count = SEQ // TOK_SP
    ranking = jax.random.permutation(level_key, block_count).astype(jnp.float32)
    levels = -1.5 + 3.0 * ranking / max(block_count - 1, 1)
    noise = jax.random.normal(noise_key, (2, HEADS, block_count, TOK_SP), jnp.float32)
    values_out = jnp.clip(noise + levels[None, None, :, None], -6.0, 6.0)
    return values_out.reshape(2, HEADS, SEQ).astype(jnp.float32)


def draw_decay_shock(key, part):
    place_key, size_key = jax.random.split(key)
    spots = jax.random.randint(place_key, (2, 2), 0, SEQ)
    amounts = jax.random.uniform(size_key, (2, HEADS, 2), jnp.float32, -0.69, -0.22)
    positions = jnp.arange(SEQ)
    marked = (positions[None, None, :] == spots[:, :, None]).astype(jnp.float32)
    return jnp.einsum('dhs,dst->dht', amounts, marked).astype(jnp.float32)


def draw_beta_pre(key, part):
    level_key, noise_key = jax.random.split(jax.random.fold_in(key, 11))
    chain_loss = jnp.exp(jax.random.uniform(level_key, (2, HEADS), jnp.float32, jnp.log(0.3), jnp.log(2.0)))
    target = chain_loss * HEAD_DIM / (2.0 * SEQ)
    level = jnp.log(target) - jnp.log1p(-target) - 0.5
    noise = jnp.clip(jax.random.normal(noise_key, (2, HEADS, SEQ), jnp.float32), -4.0, 4.0)
    return jnp.clip(level[:, :, None] + noise, -12.0, 0.0).astype(jnp.float32)


def draw_experts_pick(key, part):
    block_count = SEQ // TOK_DEV
    group_share = TOK_DEV // EXPERT_GROUPS
    order_key, swap_key = jax.random.split(key)
    ranking = jax.vmap(lambda sub_key: jax.random.permutation(sub_key, TOK_DEV))(jax.random.split(order_key, block_count))
    group_of = ranking // group_share
    swap_bits = jax.random.randint(swap_key, (block_count, TOK_DEV), 0, 2)
    group_base = group_of * GROUP_SIZE
    picks = jnp.stack([group_base + swap_bits, group_base + 1 - swap_bits], axis=-1)
    return picks.reshape(SEQ, 2).astype(jnp.int32)


def block_scale(key, shape, cuts, least, top_value):
    loudness = 1.0
    for dim, blocks in cuts:
        steps = jax.random.uniform(jax.random.fold_in(jax.random.fold_in(key, 6), dim), (blocks,), jnp.float32, least / len(cuts), top_value / len(cuts))
        loudness = loudness * jnp.repeat(jnp.exp(steps), shape[dim] // blocks).reshape((-1,) + (1,) * (len(shape) - 1 - dim))
    return loudness


def gaussian(key, shape, deviation, limit, cuts=(), kind=jnp.bfloat16):
    array = deviation * jax.random.normal(key, shape, jnp.float32)
    if cuts:
        array = array * block_scale(key, shape, cuts, -0.22, 0.18)
    return jnp.clip(array, -limit, limit).astype(kind)


def setup_inputs(seed: int = 0) -> dict:
    splits = jax.random.split(jax.random.key(seed), 19)
    return {
        "query_vectors": gaussian(splits[0], (SEQ, HEADS, HEAD_DIM), 1.0, 6.0, ((0, 4), (1, 8))),
        "key_vectors": gaussian(splits[1], (SEQ, HEADS, HEAD_DIM), 1.0, 6.0, ((0, 4), (1, 8))),
        "value_vectors": gaussian(splits[2], (SEQ, HEADS, HEAD_DIM), 1.0, 6.0, ((0, 4), (1, 8))),
        "out_gate": gaussian(splits[3], (SEQ, HEADS, HEAD_DIM), 1.0, 6.0, ((0, 4), (1, 8))),
        "decay_rate": draw_decay_rate(jax.random.fold_in(splits[18], 71), 0),
        "decay_pre": draw_decay_pre(jax.random.fold_in(splits[18], 71), 0),
        "decay_shock": draw_decay_shock(jax.random.fold_in(splits[18], 71), 0),
        "beta_pre": draw_beta_pre(jax.random.fold_in(splits[18], 71), 0),
        "head_gain": jnp.clip(1.0 + 0.18 * jax.random.normal(splits[8], (HEAD_DIM,), jnp.float32), 0.1, 1.9),
        "w_out": gaussian(splits[9], (HEADS * HEAD_DIM, D), (HEADS * HEAD_DIM) ** -0.5, 0.125, ((0, 8),)),
        "tokens": gaussian(splits[10], (SEQ, D), 1.0, 6.0, ((0, 32),)),
        "norm_gain": jnp.clip(1.0 + 0.18 * jax.random.normal(splits[11], (D,), jnp.float32), 0.1, 1.9),
        "experts_pick": draw_experts_pick(jax.random.fold_in(splits[18], 71), 0),
        "pair_logits": gaussian(splits[13], (SEQ, 2), 1.5, 6.0, ((0, 32),), jnp.float32),
        "group_logits": gaussian(splits[14], (SEQ, EXPERT_GROUPS), 1.5, 6.0, ((0, 32),), jnp.float32),
        "expert_gate": gaussian(splits[15], (EXPERTS, D, EXP_FF), D ** -0.5, 0.125, ((0, 4), (2, 8))),
        "expert_up": gaussian(splits[16], (EXPERTS, D, EXP_FF), D ** -0.5, 0.125, ((0, 4), (2, 8))),
        "expert_down": gaussian(splits[17], (EXPERTS, D, EXP_FF), (EXP_FF // 16) ** -0.5, 0.5, ((0, 4), (2, 8))),
    }


NORM_EPSILON = 1e-06
EXACT_PRECISION = lax.Precision.HIGHEST

def unit_rows(vectors):
    return vectors * lax.rsqrt(lax.optimization_barrier(jnp.sum(vectors * vectors, axis=-1, keepdims=True)) + NORM_EPSILON)

def block_sweep(queries, key_rows, value_rows, log_decay, beta_rate, start_state):
    length, value_width = value_rows.shape
    blocks = length // BLOCK
    query_blocks = queries.reshape(blocks, BLOCK, queries.shape[1])
    key_blocks = key_rows.reshape(blocks, BLOCK, key_rows.shape[1])
    value_blocks = value_rows.reshape(blocks, BLOCK, value_width)
    cumulative = jnp.cumsum(log_decay.reshape(blocks, BLOCK), axis=1)
    beta_blocks = beta_rate.reshape(blocks, BLOCK)
    position = jnp.arange(BLOCK)
    lower_mask = position[:, None] >= position[None, :]
    strict = position[:, None] > position[None, :]
    spread = cumulative[:, :, None] - cumulative[:, None, :]
    within = jnp.where(lower_mask, jnp.exp(jnp.where(lower_mask, spread, 0.0)), 0.0)
    scaled_keys = key_blocks * beta_blocks[:, :, None]
    lower_matrix = jnp.where(strict, jnp.einsum('nid,njd->nij', scaled_keys, key_blocks, precision=EXACT_PRECISION) * within, 0.0)
    identity = jnp.eye(BLOCK, dtype=jnp.float32)
    right_side = jnp.concatenate([value_blocks * beta_blocks[:, :, None], scaled_keys * jnp.exp(cumulative)[:, :, None]], axis=2)
    solved = jax.scipy.linalg.solve_triangular(lower_matrix + identity, right_side, lower=True, unit_diagonal=True)
    fresh_values = solved[:, :, :value_width]
    corrections = solved[:, :, value_width:]
    scores = jnp.einsum('nid,njd->nij', query_blocks, key_blocks, precision=EXACT_PRECISION) * within
    query_decayed = query_blocks * jnp.exp(cumulative)[:, :, None]
    block_total = cumulative[:, -1]
    decayed_keys = key_blocks * jnp.exp(block_total[:, None] - cumulative)[:, :, None]

    def advance(carried, inputs):
        values_in, fix_rows, query_in, key_in, score_in, total_in = inputs
        updated = values_in - jnp.dot(fix_rows, carried, precision=EXACT_PRECISION)
        output = jnp.dot(query_in, carried, precision=EXACT_PRECISION) + jnp.dot(score_in, updated, precision=EXACT_PRECISION)
        carried = carried * jnp.exp(total_in) + jnp.dot(key_in.T, updated, precision=EXACT_PRECISION)
        return (carried, output)
    final_state, outputs = lax.scan(advance, start_state, (fresh_values, corrections, query_decayed, decayed_keys, scores, block_total))
    return (outputs.reshape(length, value_width), final_state)

def reference(query_vectors, key_vectors, value_vectors, out_gate, decay_rate, decay_pre, decay_shock, beta_pre, head_gain, w_out, tokens, norm_gain, experts_pick, pair_logits, group_logits, expert_gate, expert_up, expert_down):
    queries = unit_rows(jnp.transpose(query_vectors.astype(jnp.float32), (1, 0, 2))) * HEAD_DIM ** (-0.5)
    keyset = unit_rows(jnp.transpose(key_vectors.astype(jnp.float32), (1, 0, 2)))
    valueset = jnp.transpose(value_vectors.astype(jnp.float32), (1, 0, 2))
    log_decay = -decay_rate[:, :, None] * jax.nn.softplus(decay_pre) + decay_shock
    beta_rate = jax.nn.sigmoid(beta_pre)
    zero_state = jnp.zeros((HEAD_DIM, HEAD_DIM), jnp.float32)

    def one_head(packed):
        query_head, key_head, value_head, decay_head, beta_head = packed
        forward_result, _ = block_sweep(query_head, key_head, value_head, decay_head[0], beta_head[0], zero_state)
        trailing_part, _ = block_sweep(query_head[::-1], key_head[::-1], value_head[::-1], decay_head[1, ::-1], beta_head[1, ::-1], zero_state)
        return forward_result + trailing_part[::-1]
    joined = lax.map(one_head, (queries, keyset, valueset, jnp.moveaxis(log_decay, 1, 0), jnp.moveaxis(beta_rate, 1, 0)))
    joined = jnp.transpose(joined, (1, 0, 2))
    head_scale = lax.rsqrt(lax.optimization_barrier(jnp.mean(joined * joined, axis=-1, keepdims=True)) + NORM_EPSILON)
    mixed_heads = (joined * head_scale * head_gain * jax.nn.silu(out_gate.astype(jnp.float32))).astype(jnp.bfloat16)
    mixed_heads = mixed_heads.reshape(SEQ, HEADS * HEAD_DIM)
    group_width = HEADS * HEAD_DIM // N_TP

    def add_heads(running, group_index):
        columns = lax.dynamic_slice_in_dim(mixed_heads, group_index * group_width, group_width, 1)
        weight_rows = lax.dynamic_slice_in_dim(w_out, group_index * group_width, group_width, 0)
        part_sum = jnp.dot(columns.astype(jnp.float32), weight_rows.astype(jnp.float32), preferred_element_type=jnp.float32).astype(jnp.bfloat16)
        return (running + lax.optimization_barrier(part_sum).astype(jnp.float32), None)
    branch_sum, _ = lax.scan(add_heads, jnp.zeros((SEQ, D), jnp.float32), jnp.arange(N_TP, dtype=jnp.int32))
    residual = tokens.astype(jnp.float32) + branch_sum
    normed = (residual * lax.rsqrt(lax.optimization_barrier(jnp.mean(residual * residual, axis=-1, keepdims=True)) + NORM_EPSILON) * norm_gain).astype(jnp.bfloat16)
    group_exp = jnp.exp(group_logits)
    group_share = group_exp / lax.optimization_barrier(jnp.sum(group_exp, axis=-1, keepdims=True))
    group_index_of = experts_pick[:, 0] // GROUP_SIZE
    group_weight = lax.optimization_barrier(jnp.sum(jnp.where(jnp.arange(EXPERT_GROUPS)[None, :] == group_index_of[:, None], group_share, 0.0), axis=1))
    pair_exp = jnp.exp(pair_logits)
    route_weight = pair_exp / lax.optimization_barrier(jnp.sum(pair_exp, axis=-1, keepdims=True)) * group_weight[:, None]
    block_count = SEQ // TOK_DEV
    expert_marks = lax.optimization_barrier(jnp.sum((experts_pick[:, :, None] == jnp.arange(EXPERTS, dtype=jnp.int32)[None, None, :]).astype(jnp.int32), axis=1))
    expert_marks = expert_marks.reshape(block_count, TOK_DEV, EXPERTS)
    earlier = (jnp.cumsum(expert_marks, axis=1) - expert_marks).reshape(SEQ, EXPERTS)
    slot_number = jnp.take_along_axis(earlier, experts_pick, axis=1)
    token_index = jnp.arange(SEQ, dtype=jnp.int32)
    slot_place = (token_index // TOK_DEV)[:, None] * CAP + slot_number
    buffer_rows = block_count * CAP
    slice_width = EXP_FF // N_TP
    sources = jnp.broadcast_to(token_index[:, None], (SEQ, 2)).reshape(-1)

    def add_expert(running, expert):
        expert_hits = experts_pick == expert
        target = jnp.where(expert_hits, slot_place, buffer_rows).reshape(-1).astype(jnp.int32)
        slot_table = jnp.zeros((buffer_rows,), jnp.int32).at[target].set(sources, mode='drop')
        picked = normed[slot_table]
        gate_out = jnp.dot(picked.astype(jnp.float32), expert_gate[expert].astype(jnp.float32), preferred_element_type=jnp.float32)
        up_out = jnp.dot(picked.astype(jnp.float32), expert_up[expert].astype(jnp.float32), preferred_element_type=jnp.float32)
        hidden = (jax.nn.silu(gate_out) * up_out).astype(jnp.bfloat16)
        down_full = expert_down[expert]

        def add_slice(partial_value, slice_index):
            hidden_part = lax.dynamic_slice_in_dim(hidden, slice_index * slice_width, slice_width, 1)
            down_part = lax.dynamic_slice_in_dim(down_full, slice_index * slice_width, slice_width, 1)
            product = lax.dot_general(hidden_part.astype(jnp.float32), down_part.astype(jnp.float32), (((1,), (1,)), ((), ())), preferred_element_type=jnp.float32).astype(jnp.bfloat16)
            return (partial_value + lax.optimization_barrier(product).astype(jnp.float32), None)
        summed_out, _ = lax.scan(add_slice, jnp.zeros((buffer_rows, D), jnp.float32), jnp.arange(N_TP, dtype=jnp.int32))
        answer = summed_out.astype(jnp.bfloat16)
        first_hit = expert_hits[:, 0]
        row_of = jnp.where(first_hit, slot_place[:, 0], slot_place[:, 1]).astype(jnp.int32)
        weight_of = jnp.where(first_hit, route_weight[:, 0], jnp.where(expert_hits[:, 1], route_weight[:, 1], 0.0))
        return (running + weight_of[:, None] * answer[row_of].astype(jnp.float32), None)
    mixture, _ = lax.scan(add_expert, jnp.zeros((SEQ, D), jnp.float32), jnp.arange(EXPERTS, dtype=jnp.int32))
    return (residual + mixture).astype(jnp.bfloat16)
```

```python
import functools

import jax
import jax.numpy as jnp
from jax import lax
from jax.experimental import pallas as pl
from jax.experimental.pallas import tpu as pltpu
from jax.sharding import PartitionSpec as P

GROUP_SIZE = 2

NORM_EPSILON = 1e-06
EXACT_PRECISION = lax.Precision.HIGHEST
F32 = jnp.float32
BF16 = jnp.bfloat16
VMEM = pl.BlockSpec(memory_space=pltpu.VMEM)
SMEM = pl.BlockSpec(memory_space=pltpu.SMEM)


def mm(left, right, contract=((1,), (0,))):
    return lax.dot_general(left, right, (contract, ((), ())), preferred_element_type=F32)


def chunk_kernel(
    heads, q_ref, k_ref, v_ref, decay_ref, beta_ref,
    base_ref, lift_ref, ends_ref,
    stack_ref, add_ref, cum_ref, total_ref, state_ref,
):
    length = q_ref.shape[0]
    width = q_ref.shape[1] // heads
    size = decay_ref.shape[1]
    chunks = length // size
    half = heads * chunks
    row = lax.broadcasted_iota(jnp.int32, (size, size), 0)
    col = lax.broadcasted_iota(jnp.int32, (size, size), 1)
    exact = functools.partial(jnp.dot, precision=EXACT_PRECISION, preferred_element_type=F32)
    ones_up = jnp.where(row <= col, 1.0, 0.0).astype(F32)
    ones_down = jnp.where(row >= col, 1.0, 0.0).astype(F32)
    cum_ref[:half, :] = exact(decay_ref[:half, :], ones_up)
    cum_ref[half:, :] = exact(decay_ref[half:, :], ones_down)
    levels = size.bit_length() - 1

    def prepare(chunk, carry):
        start = pl.multiple_of(chunk * size, size)
        rows = pl.ds(start, size)
        distance = row ^ col
        eye = row == col
        units = []
        for head in range(heads):
            lanes = slice(head * width, (head + 1) * width)
            query = q_ref[rows, lanes].astype(F32)
            query = query * lax.rsqrt(jnp.sum(query * query, axis=1, keepdims=True) + NORM_EPSILON)
            query = query * width ** (-0.5)
            key = k_ref[rows, lanes].astype(F32)
            key = key * lax.rsqrt(jnp.sum(key * key, axis=1, keepdims=True) + NORM_EPSILON)
            value = v_ref[rows, lanes].astype(F32)
            key_low = key.astype(BF16)
            gram = mm(key_low, key_low, ((1,), (1,)))
            score = mm(query.astype(BF16), key_low, ((1,), (1,)))
            for way in range(2):
                unit = (way * heads + head) * chunks + chunk
                cum_row = cum_ref[pl.ds(unit, 1), :]
                beta_row = beta_ref[pl.ds(unit, 1), :]
                cum_col = jnp.sum(jnp.where(eye, cum_row, 0.0), axis=1, keepdims=True)
                beta_col = jnp.sum(jnp.where(eye, beta_row, 0.0), axis=1, keepdims=True)
                total = cum_row[:, size - 1 :] if way == 0 else cum_row[:, :1]
                seen = row >= col if way == 0 else row <= col
                within = jnp.where(seen, jnp.exp(jnp.where(seen, cum_col - cum_row, 0.0)), 0.0)
                lower = jnp.where(eye, 0.0, gram * within * beta_col)
                decayed = jnp.exp(cum_col)
                right = jnp.concatenate([key * (beta_col * decayed), value * beta_col], axis=1)
                total_ref[pl.ds(unit, 1), :] = jnp.broadcast_to(jnp.exp(total), (1, size))
                units.append(
                    dict(
                        unit=unit, head=head, way=way, lower=lower,
                        inverse=(jnp.where(eye, 1.0, 0.0) - jnp.where(distance == 1, lower, 0.0)).astype(BF16),
                        right=right.astype(BF16),
                        score=(score * within).astype(BF16),
                        query=query * decayed,
                        key=(key * jnp.exp(total - cum_col)).astype(BF16),
                    )
                )
        for level in range(1, levels):
            here = (distance >> level) == 1
            firsts = [
                mm(item["inverse"], jnp.where(here, item["lower"], 0.0).astype(BF16)).astype(BF16)
                for item in units
            ]
            seconds = [mm(first, item["inverse"]) for first, item in zip(firsts, units)]
            for item, second in zip(units, seconds):
                item["inverse"] = (item["inverse"].astype(F32) - second).astype(BF16)
        solved = [mm(item["inverse"], item["right"]).astype(BF16) for item in units]
        outs = [mm(item["score"], both) for item, both in zip(units, solved)]
        maps = [mm(item["key"], both, ((0,), (0,))) for item, both in zip(units, solved)]
        base = [None] * heads
        for item, out, change in zip(units, outs, maps):
            unit = item["unit"]
            stack_ref[unit, :size, :] = (item["query"] - out[:, :width]).astype(BF16)
            stack_ref[unit, size:, :] = change[:, :width].astype(BF16)
            add_ref[unit] = change[:, width:]
            fresh = out[:, width:]
            head = item["head"]
            base[head] = fresh if base[head] is None else base[head] + fresh
        for head in range(heads):
            base_ref[rows, head * width : (head + 1) * width] = base[head]
        return carry

    lax.fori_loop(0, chunks, prepare, 0)

    wide_row = lax.broadcasted_iota(jnp.int32, (width, 2 * width), 0)
    wide_col = lax.broadcasted_iota(jnp.int32, (width, 2 * width), 1)
    opening = jnp.where(wide_row + width == wide_col, 1.0, 0.0).astype(F32)
    for chain in range(2 * heads):
        state_ref[chain] = opening

    def advance(step, carry):
        for way in range(2):
            chunk = step if way == 0 else chunks - 1 - step
            rows = pl.ds(pl.multiple_of(chunk * size, size), size)
            for head in range(heads):
                chain = way * heads + head
                unit = chain * chunks + chunk
                state = state_ref[chain]
                both = mm(stack_ref[unit], state.astype(BF16))
                lanes = slice(head * width, (head + 1) * width)
                base_ref[rows, lanes] += both[:size, :width]
                lift_ref[chain, rows, :] = both[:size, width:].astype(BF16)
                keep = total_ref[pl.ds(unit, 1), :width]
                state_ref[chain, :, :width] = (
                    state[:, :width] * keep - both[size:, :width] + add_ref[unit]
                )
                state_ref[chain, :, width:] = state[:, width:] * keep - both[size:, width:]
        return carry

    lax.fori_loop(0, chunks, advance, 0)
    for chain in range(2 * heads):
        ends_ref[chain] = state_ref[chain].astype(BF16)


def chunk_maps(heads, queries, keys, values, decay, beta):
    length = queries.shape[0]
    width = queries.shape[1] // heads
    units, size = decay.shape
    return pl.pallas_call(
        functools.partial(chunk_kernel, heads),
        out_shape=(
            jax.ShapeDtypeStruct((length, heads * width), F32),
            jax.ShapeDtypeStruct((2 * heads, length, width), BF16),
            jax.ShapeDtypeStruct((2 * heads, width, 2 * width), BF16),
        ),
        in_specs=[VMEM] * 5,
        out_specs=(VMEM, VMEM, VMEM),
        scratch_shapes=[
            pltpu.VMEM((units, size + width, width), BF16),
            pltpu.VMEM((units, width, width), F32),
            pltpu.VMEM((units, size), F32),
            pltpu.VMEM((units, size), F32),
            pltpu.VMEM((2 * heads, width, 2 * width), F32),
        ],
        compiler_params=pltpu.CompilerParams(vmem_limit_bytes=40 * 1024 * 1024),
        name="chunk_maps",
    )(queries, keys, values, decay, beta)


def join_kernel(heads, own_ref, all_ref, base_ref, lift_ref, gate_ref, gain_ref, mixed_ref):
    places = all_ref.shape[0]
    width = gain_ref.shape[1]
    length = base_ref.shape[0]
    own = own_ref[0]
    states = [jnp.zeros((width, width), F32) for _ in range(2 * heads)]
    for step in range(places - 1):
        for chain in range(2 * heads):
            place = step if chain < heads else places - 1 - step
            state = states[chain]
            applied = mm(all_ref[place, chain, :, width:], state.astype(BF16)) + all_ref[
                place, chain, :, :width
            ].astype(F32)
            use = place < own if chain < heads else place > own
            states[chain] = jnp.where(use, applied, state)
    lows = [state.astype(BF16) for state in states]
    tile = min(length, 256)

    def body(step, carry):
        rows = pl.ds(pl.multiple_of(step * tile, tile), tile)
        for head in range(heads):
            lanes = slice(head * width, (head + 1) * width)
            joined = (
                base_ref[rows, lanes]
                + mm(lift_ref[head, rows, :], lows[head])
                + mm(lift_ref[heads + head, rows, :], lows[heads + head])
            )
            scale = lax.rsqrt(jnp.mean(joined * joined, axis=1, keepdims=True) + NORM_EPSILON)
            gate = gate_ref[rows, lanes].astype(F32)
            silu = gate / (1.0 + jnp.exp(-gate))
            mixed_ref[rows, lanes] = (joined * scale * gain_ref[...] * silu).astype(BF16)
        return carry

    lax.fori_loop(0, length // tile, body, 0)


def join_heads(heads, own, collected, base, lift, gate, gain):
    return pl.pallas_call(
        functools.partial(join_kernel, heads),
        out_shape=jax.ShapeDtypeStruct(base.shape, BF16),
        in_specs=[SMEM] + [VMEM] * 5,
        out_specs=VMEM,
        compiler_params=pltpu.CompilerParams(vmem_limit_bytes=40 * 1024 * 1024),
        name="join_heads",
    )(own, collected, base, lift, gate, gain)


def shards(
    query_vectors,
    key_vectors,
    value_vectors,
    out_gate,
    decay_rate,
    decay_pre,
    decay_shock,
    beta_pre,
    head_gain,
    w_out,
    tokens,
    norm_gain,
    experts_pick,
    pair_logits,
    group_logits,
    expert_gate,
    expert_up,
    expert_down,
):
    length, heads, width = query_vectors.shape
    log_decay = -decay_rate[:, :, None] * jax.nn.softplus(decay_pre) + decay_shock
    beta_rate = jax.nn.sigmoid(beta_pre)
    base, lift, ends = chunk_maps(
        heads,
        query_vectors.reshape(length, heads * width),
        key_vectors.reshape(length, heads * width),
        value_vectors.reshape(length, heads * width),
        log_decay.reshape(-1, width),
        beta_rate.reshape(-1, width),
    )
    collected = lax.all_gather(ends, "sp", axis=0)
    own = lax.axis_index("sp").astype(jnp.int32).reshape(1)
    mixed_heads = join_heads(
        heads, own, collected, base, lift, out_gate.reshape(length, heads * width), head_gain[None, :]
    )
    local_rows = tokens.shape[0]
    part_sum = jnp.dot(mixed_heads, w_out, preferred_element_type=jnp.float32).astype(jnp.bfloat16)
    branch_sum = lax.psum_scatter(
        lax.optimization_barrier(part_sum).astype(jnp.float32).astype(jnp.bfloat16),
        "tp",
        scatter_dimension=0,
        tiled=True,
    ).astype(jnp.float32)
    residual = tokens.astype(jnp.float32) + branch_sum
    normed = (
        residual
        * lax.rsqrt(jnp.mean(residual * residual, axis=-1, keepdims=True) + NORM_EPSILON)
        * norm_gain
    ).astype(jnp.bfloat16)
    group_count = group_logits.shape[1]
    group_exp = jnp.exp(group_logits)
    group_share = group_exp / jnp.sum(group_exp, axis=-1, keepdims=True)
    group_index_of = experts_pick[:, 0] // GROUP_SIZE
    group_weight = jnp.sum(
        jnp.where(jnp.arange(group_count)[None, :] == group_index_of[:, None], group_share, 0.0),
        axis=1,
    )
    pair_exp = jnp.exp(pair_logits)
    route_weight = pair_exp / jnp.sum(pair_exp, axis=-1, keepdims=True) * group_weight[:, None]
    capacity = local_rows // group_count
    expert_count = lax.axis_size("sp")
    marks = (
        experts_pick[:, :, None] == jnp.arange(expert_count, dtype=jnp.int32)[None, None, :]
    ).astype(F32)
    token = jnp.arange(local_rows, dtype=jnp.int32)
    before = (token[:, None] > token[None, :]).astype(F32)
    earlier = jnp.dot(before, jnp.sum(marks, axis=1))
    slot_number = jnp.sum(marks * earlier[:, None, :], axis=2).astype(jnp.int32)
    slot_place = experts_pick * capacity + slot_number
    slot_index = jnp.arange(expert_count * capacity, dtype=jnp.int32)
    hits = slot_place[:, :, None] == slot_index[None, None, :]
    chooser = jnp.any(hits, axis=1).astype(BF16)
    weights = jnp.sum(jnp.where(hits, route_weight[:, :, None], 0.0), axis=1)
    outgoing = mm(chooser, normed, ((0,), (0,))).astype(jnp.bfloat16)
    outgoing = outgoing.reshape(expert_count, capacity, normed.shape[1])
    arrived = lax.all_to_all(outgoing, "sp", split_axis=0, concat_axis=0, tiled=True)
    source_count, slot_count, model_width = arrived.shape
    row_count = source_count * slot_count
    flat_rows = arrived.reshape(row_count, model_width)
    part_rows = lax.all_gather(flat_rows, "tp", axis=0, tiled=True)
    gate_out = jnp.dot(part_rows, expert_gate[0], preferred_element_type=jnp.float32)
    up_out = jnp.dot(part_rows, expert_up[0], preferred_element_type=jnp.float32)
    hidden = (jax.nn.silu(gate_out) * up_out).astype(jnp.bfloat16)
    product = lax.dot_general(
        hidden, expert_down[0], (((1,), (1,)), ((), ())), preferred_element_type=jnp.float32
    ).astype(jnp.bfloat16)
    summed_out = lax.psum_scatter(
        lax.optimization_barrier(product).astype(jnp.float32).astype(jnp.bfloat16),
        "tp",
        scatter_dimension=0,
        tiled=True,
    )
    expert_rows = summed_out.reshape(source_count, slot_count, model_width)
    results = lax.all_to_all(expert_rows, "sp", split_axis=0, concat_axis=0, tiled=True)
    gathered = results.reshape(expert_count * capacity, normed.shape[1])
    mixture = jnp.dot(weights, gathered.astype(F32), precision=EXACT_PRECISION)
    return (residual + mixture).astype(jnp.bfloat16)


def solution(mesh):
    return jax.shard_map(
        shards,
        mesh=mesh,
        in_specs=(
            P("sp", "tp", None),
            P("sp", "tp", None),
            P("sp", "tp", None),
            P("sp", "tp", None),
            P(None, "tp"),
            P(None, "tp", "sp"),
            P(None, "tp", "sp"),
            P(None, "tp", "sp"),
            P(),
            P("tp", None),
            P(("sp", "tp"), None),
            P(),
            P(("sp", "tp"), None),
            P(("sp", "tp"), None),
            P(("sp", "tp"), None),
            P("sp", None, "tp"),
            P("sp", None, "tp"),
            P("sp", None, "tp"),
        ),
        out_specs=P(("sp", "tp"), None),
        check_vma=False,
    )
```

```python
import functools

import jax
import jax.numpy as jnp
from jax import lax
from jax.experimental import pallas as pl
from jax.experimental.pallas import tpu as pltpu
from jax.sharding import Mesh
from jax.sharding import PartitionSpec as P

GROUP_SIZE = 2

NORM_EPSILON = 1e-06
EXACT_PRECISION = lax.Precision.HIGHEST
F32 = jnp.float32
BF16 = jnp.bfloat16
VMEM = pl.BlockSpec(memory_space=pltpu.VMEM)
SMEM = pl.BlockSpec(memory_space=pltpu.SMEM)


def mm(left, right, contract=((1,), (0,))):
    return lax.dot_general(left, right, (contract, ((), ())), preferred_element_type=F32)


def chunk_kernel(
    heads, q_ref, k_ref, v_ref, decay_ref, beta_ref,
    base_ref, lift_ref, ends_ref,
    stack_ref, add_ref, cum_ref, total_ref, state_ref,
):
    length = q_ref.shape[0]
    width = q_ref.shape[1] // heads
    size = decay_ref.shape[1]
    chunks = length // size
    half = heads * chunks
    row = lax.broadcasted_iota(jnp.int32, (size, size), 0)
    col = lax.broadcasted_iota(jnp.int32, (size, size), 1)
    exact = functools.partial(jnp.dot, precision=EXACT_PRECISION, preferred_element_type=F32)
    ones_up = jnp.where(row <= col, 1.0, 0.0).astype(F32)
    ones_down = jnp.where(row >= col, 1.0, 0.0).astype(F32)
    cum_ref[:half, :] = exact(decay_ref[:half, :], ones_up)
    cum_ref[half:, :] = exact(decay_ref[half:, :], ones_down)
    levels = size.bit_length() - 1

    def prepare(chunk, carry):
        start = pl.multiple_of(chunk * size, size)
        rows = pl.ds(start, size)
        distance = row ^ col
        eye = row == col
        units = []
        for head in range(heads):
            lanes = slice(head * width, (head + 1) * width)
            query = q_ref[rows, lanes].astype(F32)
            query = query * lax.rsqrt(jnp.sum(query * query, axis=1, keepdims=True) + NORM_EPSILON)
            query = query * width ** (-0.5)
            key = k_ref[rows, lanes].astype(F32)
            key = key * lax.rsqrt(jnp.sum(key * key, axis=1, keepdims=True) + NORM_EPSILON)
            value = v_ref[rows, lanes].astype(F32)
            key_low = key.astype(BF16)
            gram = mm(key_low, key_low, ((1,), (1,)))
            score = mm(query.astype(BF16), key_low, ((1,), (1,)))
            for way in range(2):
                unit = (way * heads + head) * chunks + chunk
                cum_row = cum_ref[pl.ds(unit, 1), :]
                beta_row = beta_ref[pl.ds(unit, 1), :]
                cum_col = jnp.sum(jnp.where(eye, cum_row, 0.0), axis=1, keepdims=True)
                beta_col = jnp.sum(jnp.where(eye, beta_row, 0.0), axis=1, keepdims=True)
                total = cum_row[:, size - 1 :] if way == 0 else cum_row[:, :1]
                seen = row >= col if way == 0 else row <= col
                within = jnp.where(seen, jnp.exp(jnp.where(seen, cum_col - cum_row, 0.0)), 0.0)
                lower = jnp.where(eye, 0.0, gram * within * beta_col)
                decayed = jnp.exp(cum_col)
                right = jnp.concatenate([key * (beta_col * decayed), value * beta_col], axis=1)
                total_ref[pl.ds(unit, 1), :] = jnp.broadcast_to(jnp.exp(total), (1, size))
                units.append(
                    dict(
                        unit=unit, head=head, way=way, lower=lower,
                        inverse=(jnp.where(eye, 1.0, 0.0) - jnp.where(distance == 1, lower, 0.0)).astype(BF16),
                        right=right.astype(BF16),
                        score=(score * within).astype(BF16),
                        query=query * decayed,
                        key=(key * jnp.exp(total - cum_col)).astype(BF16),
                    )
                )
        for level in range(1, levels):
            here = (distance >> level) == 1
            firsts = [
                mm(item["inverse"], jnp.where(here, item["lower"], 0.0).astype(BF16)).astype(BF16)
                for item in units
            ]
            seconds = [mm(first, item["inverse"]) for first, item in zip(firsts, units)]
            for item, second in zip(units, seconds):
                item["inverse"] = (item["inverse"].astype(F32) - second).astype(BF16)
        solved = [mm(item["inverse"], item["right"]).astype(BF16) for item in units]
        outs = [mm(item["score"], both) for item, both in zip(units, solved)]
        maps = [mm(item["key"], both, ((0,), (0,))) for item, both in zip(units, solved)]
        base = [None] * heads
        for item, out, change in zip(units, outs, maps):
            unit = item["unit"]
            stack_ref[unit, :size, :] = (item["query"] - out[:, :width]).astype(BF16)
            stack_ref[unit, size:, :] = change[:, :width].astype(BF16)
            add_ref[unit] = change[:, width:]
            fresh = out[:, width:]
            head = item["head"]
            base[head] = fresh if base[head] is None else base[head] + fresh
        for head in range(heads):
            base_ref[rows, head * width : (head + 1) * width] = base[head]
        return carry

    lax.fori_loop(0, chunks, prepare, 0)

    wide_row = lax.broadcasted_iota(jnp.int32, (width, 2 * width), 0)
    wide_col = lax.broadcasted_iota(jnp.int32, (width, 2 * width), 1)
    opening = jnp.where(wide_row + width == wide_col, 1.0, 0.0).astype(F32)
    for chain in range(2 * heads):
        state_ref[chain] = opening

    def advance(step, carry):
        for way in range(2):
            chunk = step if way == 0 else chunks - 1 - step
            rows = pl.ds(pl.multiple_of(chunk * size, size), size)
            for head in range(heads):
                chain = way * heads + head
                unit = chain * chunks + chunk
                state = state_ref[chain]
                both = mm(stack_ref[unit], state.astype(BF16))
                lanes = slice(head * width, (head + 1) * width)
                base_ref[rows, lanes] += both[:size, :width]
                lift_ref[chain, rows, :] = both[:size, width:].astype(BF16)
                keep = total_ref[pl.ds(unit, 1), :width]
                state_ref[chain, :, :width] = (
                    state[:, :width] * keep - both[size:, :width] + add_ref[unit]
                )
                state_ref[chain, :, width:] = state[:, width:] * keep - both[size:, width:]
        return carry

    lax.fori_loop(0, chunks, advance, 0)
    for chain in range(2 * heads):
        ends_ref[chain] = state_ref[chain].astype(BF16)


def chunk_maps(heads, queries, keys, values, decay, beta):
    length = queries.shape[0]
    width = queries.shape[1] // heads
    units, size = decay.shape
    return pl.pallas_call(
        functools.partial(chunk_kernel, heads),
        out_shape=(
            jax.ShapeDtypeStruct((length, heads * width), F32),
            jax.ShapeDtypeStruct((2 * heads, length, width), BF16),
            jax.ShapeDtypeStruct((2 * heads, width, 2 * width), BF16),
        ),
        in_specs=[VMEM] * 5,
        out_specs=(VMEM, VMEM, VMEM),
        scratch_shapes=[
            pltpu.VMEM((units, size + width, width), BF16),
            pltpu.VMEM((units, width, width), F32),
            pltpu.VMEM((units, size), F32),
            pltpu.VMEM((units, size), F32),
            pltpu.VMEM((2 * heads, width, 2 * width), F32),
        ],
        compiler_params=pltpu.CompilerParams(vmem_limit_bytes=40 * 1024 * 1024),
        name="chunk_maps",
    )(queries, keys, values, decay, beta)


def join_kernel(heads, own_ref, all_ref, base_ref, lift_ref, gate_ref, gain_ref, mixed_ref):
    places = all_ref.shape[0]
    width = gain_ref.shape[1]
    length = base_ref.shape[0]
    own = own_ref[0]
    states = [jnp.zeros((width, width), F32) for _ in range(2 * heads)]
    for step in range(places - 1):
        for chain in range(2 * heads):
            place = step if chain < heads else places - 1 - step
            state = states[chain]
            applied = mm(all_ref[place, chain, :, width:], state.astype(BF16)) + all_ref[
                place, chain, :, :width
            ].astype(F32)
            use = place < own if chain < heads else place > own
            states[chain] = jnp.where(use, applied, state)
    lows = [state.astype(BF16) for state in states]
    tile = min(length, 256)

    def body(step, carry):
        rows = pl.ds(pl.multiple_of(step * tile, tile), tile)
        for head in range(heads):
            lanes = slice(head * width, (head + 1) * width)
            joined = (
                base_ref[rows, lanes]
                + mm(lift_ref[head, rows, :], lows[head])
                + mm(lift_ref[heads + head, rows, :], lows[heads + head])
            )
            scale = lax.rsqrt(jnp.mean(joined * joined, axis=1, keepdims=True) + NORM_EPSILON)
            gate = gate_ref[rows, lanes].astype(F32)
            silu = gate / (1.0 + jnp.exp(-gate))
            mixed_ref[rows, lanes] = (joined * scale * gain_ref[...] * silu).astype(BF16)
        return carry

    lax.fori_loop(0, length // tile, body, 0)


def join_heads(heads, own, collected, base, lift, gate, gain):
    return pl.pallas_call(
        functools.partial(join_kernel, heads),
        out_shape=jax.ShapeDtypeStruct(base.shape, BF16),
        in_specs=[SMEM] + [VMEM] * 5,
        out_specs=VMEM,
        compiler_params=pltpu.CompilerParams(vmem_limit_bytes=40 * 1024 * 1024),
        name="join_heads",
    )(own, collected, base, lift, gate, gain)


def shards(
    query_vectors,
    key_vectors,
    value_vectors,
    out_gate,
    decay_rate,
    decay_pre,
    decay_shock,
    beta_pre,
    head_gain,
    w_out,
    tokens,
    norm_gain,
    experts_pick,
    pair_logits,
    group_logits,
    expert_gate,
    expert_up,
    expert_down,
):
    length, heads, width = query_vectors.shape
    log_decay = -decay_rate[:, :, None] * jax.nn.softplus(decay_pre) + decay_shock
    beta_rate = jax.nn.sigmoid(beta_pre)
    base, lift, ends = chunk_maps(
        heads,
        query_vectors.reshape(length, heads * width),
        key_vectors.reshape(length, heads * width),
        value_vectors.reshape(length, heads * width),
        log_decay.reshape(-1, width),
        beta_rate.reshape(-1, width),
    )
    collected = lax.all_gather(ends, ("grp", "mate"), axis=0)
    own = lax.axis_index(("grp", "mate")).astype(jnp.int32).reshape(1)
    mixed_heads = join_heads(
        heads, own, collected, base, lift, out_gate.reshape(length, heads * width), head_gain[None, :]
    )
    local_rows = tokens.shape[0]
    part_sum = jnp.dot(mixed_heads, w_out, preferred_element_type=jnp.float32).astype(jnp.bfloat16)
    branch_sum = lax.psum_scatter(
        lax.optimization_barrier(part_sum).astype(jnp.float32).astype(jnp.bfloat16),
        "tp",
        scatter_dimension=0,
        tiled=True,
    ).astype(jnp.float32)
    residual = tokens.astype(jnp.float32) + branch_sum
    normed = (
        residual
        * lax.rsqrt(jnp.mean(residual * residual, axis=-1, keepdims=True) + NORM_EPSILON)
        * norm_gain
    ).astype(jnp.bfloat16)
    mates = lax.axis_size("mate")
    group_count = lax.axis_size("grp")
    group_of = experts_pick[:, 0] // GROUP_SIZE
    capacity = local_rows // group_count
    member = (group_of[:, None] == jnp.arange(group_count, dtype=jnp.int32)[None, :]).astype(F32)
    token = jnp.arange(local_rows, dtype=jnp.int32)
    before = (token[:, None] > token[None, :]).astype(F32)
    rank = jnp.sum(member * jnp.dot(before, member), axis=1).astype(jnp.int32)
    place = group_of * capacity + rank
    chooser = place[:, None] == token[None, :]
    group_exp = jnp.exp(group_logits)
    group_share = group_exp / jnp.sum(group_exp, axis=-1, keepdims=True)
    group_weight = jnp.sum(member * group_share, axis=1)
    pair_exp = jnp.exp(pair_logits)
    route_weight = pair_exp / jnp.sum(pair_exp, axis=-1, keepdims=True) * group_weight[:, None]
    mate_weight = [
        jnp.sum(jnp.where(experts_pick % GROUP_SIZE == mate, route_weight, 0.0), axis=1)
        for mate in range(GROUP_SIZE)
    ]
    lane = jnp.arange(width, dtype=jnp.int32)[None, None, :]
    spread = sum(
        jnp.where(lane == mate, mate_weight[mate][:, None, None], 0.0) for mate in range(GROUP_SIZE)
    )
    slot_weight = jnp.sum(jnp.where(chooser[:, :, None], spread, 0.0), axis=0)
    all_weight = lax.all_gather(slot_weight, ("grp", "mate", "tp"), axis=0)
    tp_count = lax.axis_size("tp")
    all_weight = all_weight[:, :, :GROUP_SIZE].reshape(
        group_count, mates, tp_count, group_count, capacity, GROUP_SIZE
    )
    own_grp = lax.axis_index("grp")
    own_mate = lax.axis_index("mate")
    own_weight = lax.dynamic_index_in_dim(all_weight, own_grp, 3, keepdims=False)
    own_weight = lax.dynamic_index_in_dim(own_weight, own_mate, 4, keepdims=False)
    own_weight = jnp.transpose(own_weight, (1, 2, 0, 3)).reshape(-1, 1)
    outgoing = mm(chooser.astype(BF16), normed, ((0,), (0,))).astype(BF16)
    outgoing = outgoing.reshape(group_count, capacity, normed.shape[1])
    arrived = lax.all_to_all(outgoing, "grp", split_axis=0, concat_axis=0, tiled=True)
    flat_rows = arrived.reshape(local_rows, normed.shape[1])
    part_rows = lax.all_gather(flat_rows, ("mate", "tp"), axis=0, tiled=True)
    gate_out = jnp.dot(part_rows, expert_gate[0], preferred_element_type=F32)
    up_out = jnp.dot(part_rows, expert_up[0], preferred_element_type=F32)
    hidden = (jax.nn.silu(gate_out) * up_out * own_weight).astype(BF16)
    product = mm(hidden, expert_down[0], ((1,), (1,))).astype(BF16)
    summed_out = lax.psum_scatter(product, ("mate", "tp"), scatter_dimension=0, tiled=True)
    expert_rows = summed_out.reshape(group_count, capacity, normed.shape[1])
    results = lax.all_to_all(expert_rows, "grp", split_axis=0, concat_axis=0, tiled=True)
    gathered = results.reshape(local_rows, normed.shape[1])
    mixture = mm(chooser.astype(BF16), gathered)
    return (residual + mixture).astype(BF16)


def solution(mesh):
    places, inner = mesh.devices.shape
    mesh = Mesh(
        mesh.devices.reshape(places // GROUP_SIZE, GROUP_SIZE, inner), ("grp", "mate", "tp")
    )
    sp = ("grp", "mate")
    return jax.shard_map(
        shards,
        mesh=mesh,
        in_specs=(
            P(sp, "tp", None),
            P(sp, "tp", None),
            P(sp, "tp", None),
            P(sp, "tp", None),
            P(None, "tp"),
            P(None, "tp", sp),
            P(None, "tp", sp),
            P(None, "tp", sp),
            P(),
            P("tp", None),
            P(("grp", "mate", "tp"), None),
            P(),
            P(("grp", "mate", "tp"), None),
            P(("grp", "mate", "tp"), None),
            P(("grp", "mate", "tp"), None),
            P(sp, None, "tp"),
            P(sp, None, "tp"),
            P(sp, None, "tp"),
        ),
        out_specs=P(("grp", "mate", "tp"), None),
        check_vma=False,
    )
```
